32 devices in a mesh: sp: 8 (over z, y), tp: 4 (over x, core).
Axes of the slice: x: 2, y: 2, z: 4, core: 2. Of those that a mesh axis runs over, the one named last changes fastest.
Arguments:
- resid_in: bfloat16 [3072, 2048], P('sp'), may hold values from -6 to 6
- cotangent: bfloat16 [3072, 2048], P('sp'), may hold values from -2 to 2
- norm_gain: float32 [2048], replicated, may hold values from 0.1 to 1.9
- routes: int32 [3072, 2], P('sp'), may hold values from 0 to 7, all different within a row; in each aligned block of 384 rows (0 to 383, 384 to 767, ...) at most 192 rows name the same one
- route_weights: float32 [3072, 2], P('sp'), may hold values from 0.1 to 1
- gate_weight: bfloat16 [8, 2048, 1024], P('sp', None, 'tp'), may hold values from -0.125 to 0.125
- up_weight: bfloat16 [8, 2048, 1024], P('sp', None, 'tp'), may hold values from -0.125 to 0.125
- down_weight: bfloat16 [8, 1024, 2048], P('sp', 'tp'), may hold values from -0.1875 to 0.1875
- out_weight: bfloat16 [2048, 1024], P(None, 'tp'), may hold values from -0.1875 to 0.1875
- gate_b: bfloat16 [3072, 1024], P('sp', 'tp'), may hold values from -6 to 6
- gate_c: bfloat16 [3072, 1024], P('sp', 'tp'), may hold values from -6 to 6
- values_u: bfloat16 [3072, 1024], P('sp', 'tp'), may hold values from -6 to 6
- taps: float32 [3, 1024], P(None, 'tp'), may hold values from -3.5 to 3.5
Outputs:
- grad_gate_weight: float32 [8, 2048, 1024], P('sp', None, 'tp')
- grad_up_weight: float32 [8, 2048, 1024], P('sp', None, 'tp')
- grad_down_weight: float32 [8, 1024, 2048], P('sp', 'tp')
- grad_resid: bfloat16 [3072, 2048], P('sp')
- grad_out_weight: float32 [2048, 1024], P('sp', 'tp')
- grad_gate_b: bfloat16 [3072, 1024], P('sp', 'tp')
- grad_gate_c: bfloat16 [3072, 1024], P('sp', 'tp')
- grad_values: bfloat16 [3072, 1024], P('sp', 'tp')
The draws below stay inside these ranges and needn't reach their ends.
Inputs may be any that keep to these rules, and one draw needn't show every extreme that they name: `routes`: A row's 2 experts differ. In the rows of one index of sp (384 tokens) no expert is named more than 192 times, a bound that some block reaches.
All inputs are finite; a program needn't handle non-finite values.
Results may differ from the reference program's by a relative error of at most 0.024.
Values may be sent and summed in bfloat16 or wider, within the bound.
A program may use at most 128 MiB of HBM per device.

```python
import math
import jax
import jax.numpy as jnp
import numpy as np
from jax import lax

D = 2048
SC = 1024
FF = 1024
TAPS = 3
TOP = 2
TOK_DEV = 384
EXPERTS = 8
CAP = 192
TOKENS = 3072
N_SP = 8
N_TP = 4


def with_spikes(entries, own_key, source, target, parts, factor):
    owner, partner = [(jnp.arange(entries.shape[axis_at]) // (entries.shape[axis_at] // parts)).reshape([-1 if axis == axis_at else 1 for axis in range(entries.ndim)]) for axis_at in (source, target)]
    chosen = jax.random.permutation(own_key, parts)[partner]
    strong = (owner == chosen) | (owner == (partner + parts // 2) % parts)
    return jnp.where(strong, factor * entries, entries)


def steps_of(key, shape, split, smallest, largest):
    factor_of, own = 1.0, jax.random.fold_in(key, 6)
    for position, blocks in split:
        draws = jnp.exp(jax.random.uniform(jax.random.fold_in(own, position), (blocks,), jnp.float32, smallest / len(split), largest / len(split)))
        factor_of = factor_of * jnp.repeat(draws, shape[position] // blocks).reshape([-1 if axis == position else 1 for axis in range(len(shape))])
    return factor_of


def deal_out(rng, own, number, rows, number_of, top, most, skew):
    sequence = jax.random.permutation(rng, number_of)
    heavy_load, common = shares(number_of, rows * top, most, skew, True), shares(number_of, rows * top, most, skew, False)
    places = jnp.arange(number_of)

    def named(tallies, rotation):
        used = int((tallies > 0).sum())
        fixed = max(1, used // 4)
        passed = fixed + (places - fixed + rotation * (used - fixed)) % max(1, number_of - fixed)
        return jnp.zeros((number_of,), jnp.int32).at[sequence[jnp.where(places < fixed, places, passed)]].set(jnp.asarray(tallies, jnp.int32))

    tallies = jnp.where(number % 4 == 0, named(heavy_load, number // 4), named(common, number - number // 4 - 1))
    mixed = jax.random.permutation(jax.random.fold_in(own, 3), number_of)
    source_of, receiver = mixed[0:number_of // 2 * 2:2], mixed[1:number_of // 2 * 2:2]
    room = jnp.minimum(tallies[source_of] - 1, most - tallies[receiver]) // 2
    room = jnp.where((source_of == sequence[0]) | (receiver == sequence[0]) | (tallies[receiver] == 0), 0, jnp.maximum(room, 0))
    passed = jax.random.randint(jax.random.fold_in(own, 4), (number_of // 2,), 0, 1 << 20) % (room + 1)
    tallies = tallies.at[source_of].add(-passed).at[receiver].add(passed)
    items = jnp.searchsorted(jnp.cumsum(tallies), jnp.arange(rows * top), side="right").astype(jnp.int32)
    listing = items.reshape(top, rows).T
    listing = listing[jax.random.permutation(jax.random.fold_in(own, 1), rows)]
    rotation = jax.random.randint(jax.random.fold_in(own, 2), (rows, 1), 0, top)
    return jnp.take_along_axis(listing, (jnp.arange(top)[None, :] + rotation) % top, axis=1)


def shares(number_of, total, reach, slope, full):
    portions = [(1 << 20) // math.isqrt(grade ** slope) + 1 for grade in range(1, number_of + 1)]
    largest = reach if full else min(reach, max(-(-total // number_of), total * portions[0] // sum(portions)))
    least = 1 if total - largest >= number_of - 1 else 0
    given, surplus = [largest] + [least] * (number_of - 1), total - largest - least * (number_of - 1)
    while surplus > 0:
        free = [i for i in range(1, number_of) if given[i] < largest] or [i for i in range(1, number_of) if given[i] < reach]
        pool, remaining = sum([portions[i] for i in free]), surplus
        for i in free:
            more = min(reach - given[i], max(1, remaining * portions[i] // pool), surplus)
            given[i] = given[i] + more
            surplus = surplus - more
    return np.array(given)


def gaussian(stream_key, extent, scale, reach, cuts=(), held_as=jnp.bfloat16):
    result = jax.random.normal(stream_key, extent, jnp.float32) * scale
    if len(cuts) > 0:
        result = steps_of(stream_key, extent, cuts, -0.22, 0.18) * result
    return jnp.clip(result, min=-reach, max=reach).astype(held_as)


def bell_draw_with(key, dims, spread, reach, pieces, heavy, held_as=jnp.bfloat16):
    drawn = spread * jax.random.normal(key, dims, jnp.float32)
    if pieces:
        drawn = drawn * steps_of(key, dims, pieces, -0.22, 0.18)
    return jnp.clip(with_spikes(drawn, jax.random.fold_in(key, 3), *heavy), -reach, reach).astype(held_as)


def setup_inputs(seed: int = 0) -> dict:
    arg_keys = jax.random.split(jax.random.key(seed), 14)
    resid_in = gaussian(arg_keys[0], (TOKENS, D), 1.0, 6.0, ((0, 8),))
    cotangent = bell_draw_with(arg_keys[1], (TOKENS, D), 0.25, 2.0, ((0, 8),), (0, 1, 8, 2.0))
    norm_gain = jnp.clip(1.0 + 0.18 * jax.random.normal(arg_keys[2], (D,), jnp.float32), 0.1, 1.9)
    routes_keys = jax.random.split(jax.random.fold_in(arg_keys[3], 1), TOKENS // TOK_DEV)
    routes_turns = jax.random.permutation(jax.random.fold_in(arg_keys[3], 3), TOKENS // TOK_DEV)
    routes = jax.vmap(lambda own, number: deal_out(jax.random.fold_in(arg_keys[3], 2), own, number, TOK_DEV, EXPERTS, TOP, CAP, 1))(routes_keys, routes_turns).reshape((TOKENS, TOP))
    route_weights = jnp.clip(0.1 + 0.9 * jax.random.uniform(arg_keys[4], (TOKENS, TOP), jnp.float32) ** steps_of(arg_keys[4], (TOKENS, TOP), ((0, 8),), -0.2, 0.2), 0.1, 1.0)
    gate_weight = gaussian(arg_keys[5], (EXPERTS, D, FF), D ** -0.5, 0.125, ((0, 8), (2, 4)))
    up_weight = gaussian(arg_keys[6], (EXPERTS, D, FF), D ** -0.5, 0.125, ((0, 8), (2, 4)))
    down_weight = gaussian(arg_keys[7], (EXPERTS, FF, D), FF ** -0.5, 0.1875, ((0, 8), (1, 4)))
    out_weight = gaussian(arg_keys[8], (D, SC), SC ** -0.5, 0.1875, ((1, 4),))
    gate_b = gaussian(arg_keys[9], (TOKENS, SC), 1.0, 6.0, ((0, 8), (1, 4)))
    gate_c = gaussian(arg_keys[10], (TOKENS, SC), 1.0, 6.0, ((0, 8), (1, 4)))
    values_u = gaussian(arg_keys[11], (TOKENS, SC), 1.0, 6.0, ((0, 8), (1, 4)))
    taps = gaussian(arg_keys[12], (TAPS, SC), TAPS ** -0.5, 3.5, ((1, 4),), jnp.float32)
    return dict(resid_in=resid_in, cotangent=cotangent, norm_gain=norm_gain, routes=routes, route_weights=route_weights, gate_weight=gate_weight, up_weight=up_weight, down_weight=down_weight, out_weight=out_weight, gate_b=gate_b, gate_c=gate_c, values_u=values_u, taps=taps)


norm_eps = 1e-06

def expert_pass(entry_rows, entry_cots, entry_weights, gate_mat, up_mat, down_mat):
    f32 = jnp.float32
    bf16 = jnp.bfloat16
    gate_pre = jnp.dot(entry_rows, gate_mat, preferred_element_type=f32)
    up_pre = jnp.dot(entry_rows, up_mat, preferred_element_type=f32)
    logistic = jax.nn.sigmoid(gate_pre)
    activated = gate_pre * logistic
    hidden = (activated * up_pre * entry_weights[:, None]).astype(bf16)
    grad_down = jnp.dot(hidden.T, entry_cots, preferred_element_type=f32)
    dhidden = jnp.dot(entry_cots, down_mat.T, preferred_element_type=f32) * entry_weights[:, None]
    dgate = (dhidden * up_pre * logistic * (1.0 + gate_pre * (1.0 - logistic))).astype(bf16)
    dup = (dhidden * activated).astype(bf16)
    grad_gate = jnp.dot(entry_rows.T, dgate, preferred_element_type=f32)
    grad_up = jnp.dot(entry_rows.T, dup, preferred_element_type=f32)
    quarter = gate_mat.shape[1] // N_TP
    summed = jnp.zeros((entry_rows.shape[0], entry_rows.shape[1]), f32)
    for lane_index in range(N_TP):
        lower = lane_index * quarter
        upper = lower + quarter
        partial_sum = jnp.dot(dgate[:, lower:upper], gate_mat[:, lower:upper].T, preferred_element_type=f32) + jnp.dot(dup[:, lower:upper], up_mat[:, lower:upper].T, preferred_element_type=f32)
        summed = summed + lax.optimization_barrier(partial_sum.astype(bf16)).astype(f32)
    return (grad_gate, grad_up, grad_down, summed.astype(bf16))

def reference(resid_in, cotangent, norm_gain, routes, route_weights, gate_weight, up_weight, down_weight, out_weight, gate_b, gate_c, values_u, taps):
    f32 = jnp.float32
    bf16 = jnp.bfloat16
    token_total = resid_in.shape[0]
    resid_wide = resid_in.astype(f32)
    inv_rms = lax.rsqrt(lax.optimization_barrier(jnp.mean(resid_wide * resid_wide, axis=1, keepdims=True)) + norm_eps)
    normed = (resid_wide * inv_rms * norm_gain).astype(bf16)
    flat_routes = routes.reshape(-1).astype(jnp.int32)
    flat_weights = route_weights.reshape(-1)
    slot_total = N_SP * CAP

    def one_expert(expert_id):
        chosen = flat_routes == expert_id
        found = jnp.nonzero(chosen, size=slot_total, fill_value=0)[0].astype(jnp.int32)
        how_many = jnp.sum(chosen.astype(jnp.int32))
        is_valid = jnp.arange(slot_total, dtype=jnp.int32) < how_many
        owners = found // 2
        entry_weights = jnp.where(is_valid, flat_weights[found], jnp.zeros((), f32))
        grads = expert_pass(normed[owners], cotangent[owners], entry_weights, gate_weight[expert_id], up_weight[expert_id], down_weight[expert_id])
        targets = jnp.where(is_valid, found, 2 * token_total).astype(jnp.int32)
        return (grads[0], grads[1], grads[2], grads[3], targets)
    grad_gate_weight, grad_up_weight, grad_down_weight, slot_rows, targets = lax.map(one_expert, jnp.arange(EXPERTS, dtype=jnp.int32))
    slot_grads = jnp.zeros((2 * token_total + 1, D), f32).at[targets.reshape(-1)].add(slot_rows.reshape(-1, D).astype(f32))
    paired = slot_grads[:2 * token_total].reshape(token_total, 2, D)
    dnormed = paired[:, 0] + paired[:, 1]
    scaled = dnormed * norm_gain
    resid_grad = cotangent.astype(f32) + inv_rms * scaled - resid_wide * inv_rms ** 3 * lax.optimization_barrier(jnp.mean(scaled * resid_wide, axis=1, keepdims=True))
    grad_resid = resid_grad.astype(bf16)
    mixed = gate_c.astype(f32) * values_u.astype(f32)
    padded = jnp.pad(mixed, ((2, 0), (0, 0)))
    conv = taps[0] * padded[:-2] + taps[1] * padded[1:-1] + taps[2] * padded[2:]
    merged = (gate_b.astype(f32) * conv).astype(bf16)
    grad_out_weight = jnp.dot(grad_resid.T, merged, preferred_element_type=f32)
    dmerged = jnp.dot(grad_resid, out_weight, preferred_element_type=f32)
    grad_gate_b = (dmerged * conv).astype(bf16)
    dconv = dmerged * gate_b.astype(f32)
    padded_grad = jnp.pad(dconv, ((0, 2), (0, 0)))
    dmixed = taps[2] * padded_grad[:-2] + taps[1] * padded_grad[1:-1] + taps[0] * padded_grad[2:]
    grad_gate_c = (dmixed * values_u.astype(f32)).astype(bf16)
    grad_values = (dmixed * gate_c.astype(f32)).astype(bf16)
    return (grad_gate_weight, grad_up_weight, grad_down_weight, grad_resid, grad_out_weight, grad_gate_b, grad_gate_c, grad_values)
```

```python
import jax
import jax.numpy as jnp
from jax import lax
from jax.sharding import PartitionSpec as P

norm_eps = 1e-06


def passed_along(array, axis, by):
    size = lax.axis_size(axis)
    pairs = [(i, i + by) for i in range(size) if 0 <= i + by < size]
    return lax.ppermute(array, axis, pairs)


def expert_pass(entry_rows, entry_cots, entry_weights, gate_mat, up_mat, down_mat):
    f32 = jnp.float32
    bf16 = jnp.bfloat16
    gate_pre = jnp.dot(entry_rows, gate_mat, preferred_element_type=f32)
    up_pre = jnp.dot(entry_rows, up_mat, preferred_element_type=f32)
    logistic = jax.nn.sigmoid(gate_pre)
    activated = gate_pre * logistic
    hidden = (activated * up_pre * entry_weights[:, None]).astype(bf16)
    grad_down = jnp.einsum("rf,rd->fd", hidden, entry_cots, preferred_element_type=f32)
    dhidden = (
        jnp.einsum("rd,fd->rf", entry_cots, down_mat, preferred_element_type=f32)
        * entry_weights[:, None]
    )
    dgate = (dhidden * up_pre * logistic * (1.0 + gate_pre * (1.0 - logistic))).astype(bf16)
    dup = (dhidden * activated).astype(bf16)
    grad_gate = jnp.einsum("rd,rf->df", entry_rows, dgate, preferred_element_type=f32)
    grad_up = jnp.einsum("rd,rf->df", entry_rows, dup, preferred_element_type=f32)
    partial_sum = jnp.einsum("rf,df->rd", dgate, gate_mat, preferred_element_type=f32) + jnp.einsum(
        "rf,df->rd", dup, up_mat, preferred_element_type=f32
    )
    return (grad_gate, grad_up, grad_down, partial_sum)


def on_device(
    resid_in,
    cotangent,
    norm_gain,
    routes,
    route_weights,
    gate_weight,
    up_weight,
    down_weight,
    out_weight,
    gate_b,
    gate_c,
    values_u,
    taps,
):
    f32 = jnp.float32
    bf16 = jnp.bfloat16
    token_count, model_width = resid_in.shape
    groups = lax.axis_size("sp")
    lanes = lax.axis_size("tp")
    local_experts = gate_weight.shape[0]
    expert_total = local_experts * groups
    capacity = 4 * token_count // expert_total
    slot_span = local_experts * capacity
    resid_wide = resid_in.astype(f32)
    inv_rms = lax.rsqrt(jnp.mean(resid_wide * resid_wide, axis=1, keepdims=True) + norm_eps)
    normed = (resid_wide * inv_rms * norm_gain).astype(bf16)
    mixed = gate_c.astype(f32) * values_u.astype(f32)
    earlier = passed_along(mixed[-2:], "sp", 1)
    quarter = model_width // lanes
    lane = lax.axis_index("tp")
    slots = expert_total * capacity
    names = jnp.arange(expert_total, dtype=jnp.int32)
    chosen = routes[:, :, None] == names[None, None, :]
    named = jnp.any(chosen, axis=1).astype(bf16)
    order = jnp.arange(token_count, dtype=jnp.int32)
    strict = (order[:, None] > order[None, :]).astype(bf16)
    before = jnp.dot(strict, named, preferred_element_type=f32).astype(jnp.int32)
    rank = jnp.sum(jnp.where(chosen, before[:, None, :], 0), axis=2)
    targets = routes * capacity + rank
    slot_ids = jnp.arange(slots, dtype=jnp.int32)[:, None]
    first = slot_ids == targets[:, 0][None, :]
    second = slot_ids == targets[:, 1][None, :]
    placing = (first | second).astype(bf16)
    sent_weights = jnp.sum(
        jnp.where(first, route_weights[:, 0][None, :], 0.0)
        + jnp.where(second, route_weights[:, 1][None, :], 0.0),
        axis=1,
    ).reshape(groups, slot_span)
    own_rows = lax.dynamic_slice_in_dim(normed, lane * quarter, quarter, axis=1)
    own_cots = lax.dynamic_slice_in_dim(cotangent, lane * quarter, quarter, axis=1)
    sent_rows = jnp.dot(placing, own_rows, preferred_element_type=f32).astype(bf16)
    sent_cots = jnp.dot(placing, own_cots, preferred_element_type=f32).astype(bf16)
    sent_rows = sent_rows.reshape(groups, slot_span, quarter)
    sent_cots = sent_cots.reshape(groups, slot_span, quarter)
    got_weights = lax.all_to_all(sent_weights, "sp", split_axis=0, concat_axis=0, tiled=True)
    got_rows = lax.all_gather(
        lax.all_to_all(sent_rows, "sp", split_axis=0, concat_axis=0, tiled=True),
        "tp", axis=2, tiled=True,
    )
    got_cots = lax.all_gather(
        lax.all_to_all(sent_cots, "sp", split_axis=0, concat_axis=0, tiled=True),
        "tp", axis=2, tiled=True,
    )
    grads_gate, grads_up, grads_down, terms = ([], [], [], [])
    entry_rows = got_rows.reshape(groups * capacity, model_width)
    entry_cots = got_cots.reshape(groups * capacity, model_width)
    entry_weights = got_weights.reshape(groups * capacity)
    grad_gate, grad_up, grad_down, partial_sum = expert_pass(
        entry_rows, entry_cots, entry_weights, gate_weight[0], up_weight[0], down_weight[0]
    )
    grads_gate.append(grad_gate)
    grads_up.append(grad_up)
    grads_down.append(grad_down)
    terms.append(partial_sum.astype(bf16).reshape(groups, capacity, model_width))
    expert_term = terms[0]
    summed = (
        lax.psum_scatter(expert_term, "tp", scatter_dimension=2, tiled=True)
        .astype(jnp.float32)
        .astype(bf16)
    )
    returned = lax.all_to_all(summed, "sp", split_axis=0, concat_axis=0, tiled=True).reshape(
        expert_total * capacity, model_width // lanes
    )
    own_grad = jnp.einsum("st,sq->tq", placing, returned, preferred_element_type=f32)
    dnormed = lax.all_gather(own_grad.astype(bf16), "tp", axis=1, tiled=True).astype(f32)
    scaled = dnormed * norm_gain
    resid_grad = (
        cotangent.astype(f32)
        + inv_rms * scaled
        - resid_wide * inv_rms**3 * jnp.mean(scaled * resid_wide, axis=1, keepdims=True)
    )
    grad_resid = resid_grad.astype(bf16)
    extended = jnp.concatenate([earlier, mixed], axis=0)
    conv = (
        taps[0] * extended[:token_count]
        + taps[1] * extended[1 : token_count + 1]
        + taps[2] * extended[2 : token_count + 2]
    )
    merged = (gate_b.astype(f32) * conv).astype(bf16)
    grad_out_weight = lax.psum_scatter(
        jnp.einsum("td,tc->dc", grad_resid, merged, preferred_element_type=f32).astype(
            jnp.bfloat16
        ),
        "sp",
        scatter_dimension=0,
        tiled=True,
    ).astype(jnp.float32)
    dmerged = jnp.dot(grad_resid, out_weight, preferred_element_type=f32)
    grad_gate_b = (dmerged * conv).astype(bf16)
    dconv = dmerged * gate_b.astype(f32)
    later = passed_along(dconv[:2], "sp", -1)
    extended_grad = jnp.concatenate([dconv, later], axis=0)
    dmixed = (
        taps[2] * extended_grad[:token_count]
        + taps[1] * extended_grad[1 : token_count + 1]
        + taps[0] * extended_grad[2 : token_count + 2]
    )
    grad_gate_c = (dmixed * values_u.astype(f32)).astype(bf16)
    grad_values = (dmixed * gate_c.astype(f32)).astype(bf16)
    return (
        jnp.stack(grads_gate),
        jnp.stack(grads_up),
        jnp.stack(grads_down),
        grad_resid,
        grad_out_weight,
        grad_gate_b,
        grad_gate_c,
        grad_values,
    )


def solution(mesh):
    placed = (
        P("sp", None),
        P("sp", None),
        P(),
        P("sp", None),
        P("sp", None),
        P("sp", None, "tp"),
        P("sp", None, "tp"),
        P("sp", "tp", None),
        P(None, "tp"),
        P("sp", "tp"),
        P("sp", "tp"),
        P("sp", "tp"),
        P(None, "tp"),
    )
    return jax.shard_map(
        on_device,
        mesh=mesh,
        in_specs=placed,
        out_specs=(
            P("sp", None, "tp"),
            P("sp", None, "tp"),
            P("sp", "tp", None),
            P("sp", None),
            P("sp", "tp"),
            P("sp", "tp"),
            P("sp", "tp"),
            P("sp", "tp"),
        ),
        check_vma=False,
    )
```

```python
import functools

import jax
import jax.numpy as jnp
from jax import lax
from jax.experimental import pallas as pl
from jax.experimental.pallas import tpu as pltpu
from jax.sharding import PartitionSpec as P

norm_eps = 1e-06


def passed_along(array, axis, by):
    size = lax.axis_size(axis)
    pairs = [(i, i + by) for i in range(size) if 0 <= i + by < size]
    return lax.ppermute(array, axis, pairs)


def remote(source, target, send_sem, recv_sem, **device):
    return pltpu.make_async_remote_copy(
        src_ref=source,
        dst_ref=target,
        send_sem=send_sem,
        recv_sem=recv_sem,
        device_id=device,
        device_id_type=pl.DeviceIdType.MESH,
    )


def greet(groups, spot, core_peer, far_peer):
    barrier = pltpu.get_barrier_semaphore()

    def to_group(offset, carry):
        pl.semaphore_signal(
            barrier,
            inc=1,
            device_id={"sp": lax.rem(spot + offset, groups)},
            device_id_type=pl.DeviceIdType.MESH,
        )
        return carry

    lax.fori_loop(1, groups, to_group, 0)
    for peer in (core_peer, far_peer):
        pl.semaphore_signal(
            barrier, inc=1, device_id={"tp": peer}, device_id_type=pl.DeviceIdType.MESH
        )
    pl.semaphore_wait(barrier, groups + 1)


def dispatch_kernel(
    groups,
    lanes,
    sent_rows,
    sent_cots,
    sent_weights,
    got_rows,
    got_cots,
    got_weights,
    local_sem,
    send_a,
    recv_a,
    send_x,
    recv_x,
    send_c,
    recv_c,
    send_f,
    recv_f,
    send_w,
    recv_w,
):
    spot, lane = lax.axis_index("sp"), lax.axis_index("tp")
    core_peer = lane + 1 - 2 * lax.rem(lane, 2)
    far_peer = lax.rem(lane + lanes // 2, lanes)
    quarter = sent_rows.shape[2]
    pairs = ((sent_rows, got_rows), (sent_cots, got_cots))

    def part(ref, block, who):
        return ref.at[block, :, pl.ds(pl.multiple_of(who * quarter, quarter), quarter)]

    def across(k, offset):
        goal = lax.rem(spot + offset, groups)
        return remote(
            pairs[k][0].at[goal],
            part(pairs[k][1], spot, lane),
            send_a.at[k, offset],
            recv_a.at[k, offset],
            sp=goal,
        )

    def weights_across(offset):
        goal = lax.rem(spot + offset, groups)
        return remote(
            sent_weights.at[goal],
            got_weights.at[spot],
            send_w.at[offset],
            recv_w.at[offset],
            sp=goal,
        )

    def origin(offset):
        return lax.rem(spot - offset + groups, groups)

    def sideways(k, offset, source, far):
        sems = (send_x, recv_x) if far else (send_c, recv_c)
        return remote(
            source,
            part(pairs[k][1], origin(offset), lane),
            sems[0].at[k, offset],
            sems[1].at[k, offset],
            tp=far_peer if far else core_peer,
        )

    def forward(k, offset):
        held = part(pairs[k][1], origin(offset), far_peer)
        return remote(held, held, send_f.at[k, offset], recv_f.at[k, offset], tp=core_peer)

    greet(groups, spot, core_peer, far_peer)
    own = [
        pltpu.make_async_copy(
            pairs[k][0].at[spot], part(pairs[k][1], spot, lane), local_sem.at[k]
        )
        for k in (0, 1)
    ]
    own_weights = pltpu.make_async_copy(
        sent_weights.at[spot], got_weights.at[spot], local_sem.at[2]
    )

    def launch(offset, carry):
        weights_across(offset).start()
        for k in (0, 1):
            across(k, offset).start()
        return carry

    lax.fori_loop(1, groups, launch, 0)
    for k in (0, 1):
        for far in (True, False):
            sideways(k, 0, pairs[k][0].at[spot], far).start()
    for copy in own:
        copy.start()
    own_weights.start()

    def pass_on(offset, carry):
        for k in (0, 1):
            across(k, offset).wait_recv()
            for far in (True, False):
                sideways(k, offset, part(pairs[k][1], origin(offset), lane), far).start()
        for k in (0, 1):
            sideways(k, offset - 1, part(pairs[k][1], origin(offset - 1), lane), True).wait_recv()
            forward(k, offset - 1).start()
        return carry

    lax.fori_loop(1, groups, pass_on, 0)
    for k in (0, 1):
        last = groups - 1
        sideways(k, last, part(pairs[k][1], origin(last), lane), True).wait_recv()
        forward(k, last).start()

    def finish(offset, carry):
        for k in (0, 1):
            mine = part(pairs[k][1], origin(offset), lane)
            sideways(k, offset, mine, True).wait_send()
            sideways(k, offset, mine, False).wait()
            forward(k, offset).wait()
        return carry

    def finish_across(offset, carry):
        weights_across(offset).wait()
        for k in (0, 1):
            across(k, offset).wait_send()
        return carry

    lax.fori_loop(0, groups, finish, 0)
    lax.fori_loop(1, groups, finish_across, 0)
    for copy in own:
        copy.wait()
    own_weights.wait()


def dispatch(sent_rows, sent_cots, sent_weights, groups, lanes):
    span, quarter = sent_rows.shape[1:]
    whole = jax.ShapeDtypeStruct((groups, span, quarter * lanes), sent_rows.dtype)
    sem = pltpu.SemaphoreType.DMA
    anywhere = pl.BlockSpec(memory_space=pl.ANY)
    wire = 2 * span * quarter * 2 * groups * 3
    return pl.pallas_call(
        functools.partial(dispatch_kernel, groups, lanes),
        out_shape=(
            whole,
            whole,
            jax.ShapeDtypeStruct(sent_weights.shape, sent_weights.dtype),
        ),
        in_specs=[anywhere] * 3,
        out_specs=(anywhere,) * 3,
        scratch_shapes=[sem((3,))] + [sem((2, groups))] * 8 + [sem((groups,))] * 2,
        compiler_params=pltpu.CompilerParams(collective_id=1, has_side_effects=True),
        cost_estimate=pl.CostEstimate(
            flops=0, bytes_accessed=40 * wire, transcendentals=0
        ),
        name="dispatch",
    )(sent_rows, sent_cots, sent_weights)


def collect_kernel(
    groups,
    lanes,
    partial,
    returned,
    from_core,
    to_far,
    from_far,
    summed,
    send_c,
    recv_c,
    send_x,
    recv_x,
    send_a,
    recv_a,
):
    f32 = jnp.float32
    bf16 = jnp.bfloat16
    spot, lane = lax.axis_index("sp"), lax.axis_index("tp")
    core_peer = lane + 1 - 2 * lax.rem(lane, 2)
    far_peer = lax.rem(lane + lanes // 2, lanes)
    quarter = returned.shape[2]

    def part(block, who):
        return partial.at[block, :, pl.ds(pl.multiple_of(who * quarter, quarter), quarter)]

    def goal_of(step):
        return lax.rem(spot + step + 1, groups)

    def to_core(step, far):
        who = lax.rem(core_peer + far * (lanes // 2), lanes)
        return remote(
            part(goal_of(step), who),
            from_core.at[step, far],
            send_c.at[step, far],
            recv_c.at[step, far],
            tp=core_peer,
        )

    def to_far_peer(step):
        return remote(
            to_far.at[step], from_far.at[step], send_x.at[step], recv_x.at[step], tp=far_peer
        )

    def home(step):
        goal = goal_of(step)
        return remote(
            summed.at[step], returned.at[spot], send_a.at[step], recv_a.at[step], sp=goal
        )

    greet(groups, spot, core_peer, far_peer)

    def begin(step, carry):
        to_core(step, 1).start()
        to_core(step, 0).start()
        return carry

    lax.fori_loop(0, groups, begin, 0)

    def middle(step, carry):
        to_core(step, 1).wait_recv()
        to_far[step] = (
            part(goal_of(step), far_peer)[...].astype(f32) + from_core[step, 1].astype(f32)
        ).astype(bf16)
        to_far_peer(step).start()
        return carry

    lax.fori_loop(0, groups, middle, 0)

    def total(step):
        to_core(step, 0).wait_recv()
        to_far_peer(step).wait_recv()
        return (
            part(goal_of(step), lane)[...].astype(f32)
            + from_core[step, 0].astype(f32)
            + from_far[step].astype(f32)
        ).astype(bf16)

    def end(step, carry):
        summed[step] = total(step)
        home(step).start()
        return carry

    lax.fori_loop(0, groups - 1, end, 0)
    returned[spot] = total(groups - 1)

    def finish(step, carry):
        to_core(step, 0).wait_send()
        to_core(step, 1).wait_send()
        to_far_peer(step).wait_send()
        return carry

    lax.fori_loop(0, groups, finish, 0)

    def finish_home(step, carry):
        home(step).wait()
        return carry

    lax.fori_loop(0, groups - 1, finish_home, 0)


def collect(partial, groups, lanes):
    span, width = partial.shape[1:]
    quarter = width // lanes
    block = (groups, span, quarter)
    sem = pltpu.SemaphoreType.DMA
    inside = pl.BlockSpec(memory_space=pltpu.VMEM)
    return pl.pallas_call(
        functools.partial(collect_kernel, groups, lanes),
        out_shape=jax.ShapeDtypeStruct(block, partial.dtype),
        in_specs=[inside],
        out_specs=inside,
        scratch_shapes=[
            pltpu.VMEM((groups, 2, span, quarter), partial.dtype),
            pltpu.VMEM(block, partial.dtype),
            pltpu.VMEM(block, partial.dtype),
            pltpu.VMEM(block, partial.dtype),
            sem((groups, 2)),
            sem((groups, 2)),
        ]
        + [sem((groups,))] * 4,
        compiler_params=pltpu.CompilerParams(
            collective_id=2, has_side_effects=True, vmem_limit_bytes=40 * 2**20
        ),
        cost_estimate=pl.CostEstimate(
            flops=0, bytes_accessed=150 * 2**20, transcendentals=0
        ),
        name="collect",
    )(partial)


def expert_pass(entry_rows, entry_cots, entry_weights, gate_mat, up_mat, down_mat):
    f32 = jnp.float32
    bf16 = jnp.bfloat16
    gate_pre = jnp.dot(entry_rows, gate_mat, preferred_element_type=f32)
    up_pre = jnp.dot(entry_rows, up_mat, preferred_element_type=f32)
    logistic = jax.nn.sigmoid(gate_pre)
    activated = gate_pre * logistic
    hidden = (activated * up_pre * entry_weights[:, None]).astype(bf16)
    grad_down = jnp.einsum("rf,rd->fd", hidden, entry_cots, preferred_element_type=f32)
    dhidden = (
        jnp.einsum("rd,fd->rf", entry_cots, down_mat, preferred_element_type=f32)
        * entry_weights[:, None]
    )
    dgate = (dhidden * up_pre * logistic * (1.0 + gate_pre * (1.0 - logistic))).astype(bf16)
    dup = (dhidden * activated).astype(bf16)
    grad_gate = jnp.einsum("rd,rf->df", entry_rows, dgate, preferred_element_type=f32)
    grad_up = jnp.einsum("rd,rf->df", entry_rows, dup, preferred_element_type=f32)
    partial_sum = jnp.einsum("rf,df->rd", dgate, gate_mat, preferred_element_type=f32) + jnp.einsum(
        "rf,df->rd", dup, up_mat, preferred_element_type=f32
    )
    return (grad_gate, grad_up, grad_down, partial_sum)


def on_device(
    resid_in,
    cotangent,
    norm_gain,
    routes,
    route_weights,
    gate_weight,
    up_weight,
    down_weight,
    out_weight,
    gate_b,
    gate_c,
    values_u,
    taps,
):
    f32 = jnp.float32
    bf16 = jnp.bfloat16
    token_count, model_width = resid_in.shape
    groups = lax.axis_size("sp")
    lanes = lax.axis_size("tp")
    local_experts = gate_weight.shape[0]
    expert_total = local_experts * groups
    capacity = 4 * token_count // expert_total
    slot_span = local_experts * capacity
    resid_wide = resid_in.astype(f32)
    inv_rms = lax.rsqrt(jnp.mean(resid_wide * resid_wide, axis=1, keepdims=True) + norm_eps)
    normed = (resid_wide * inv_rms * norm_gain).astype(bf16)
    mixed = gate_c.astype(f32) * values_u.astype(f32)
    earlier = passed_along(mixed[-2:], "sp", 1)
    quarter = model_width // lanes
    lane = lax.axis_index("tp")
    slots = expert_total * capacity
    names = jnp.arange(expert_total, dtype=jnp.int32)
    chosen = routes[:, :, None] == names[None, None, :]
    named = jnp.any(chosen, axis=1).astype(bf16)
    order = jnp.arange(token_count, dtype=jnp.int32)
    strict = (order[:, None] > order[None, :]).astype(bf16)
    before = jnp.dot(strict, named, preferred_element_type=f32).astype(jnp.int32)
    rank = jnp.sum(jnp.where(chosen, before[:, None, :], 0), axis=2)
    targets = routes * capacity + rank
    slot_ids = jnp.arange(slots, dtype=jnp.int32)[:, None]
    first = slot_ids == targets[:, 0][None, :]
    second = slot_ids == targets[:, 1][None, :]
    placing = (first | second).astype(bf16)
    sent_weights = jnp.sum(
        jnp.where(first, route_weights[:, 0][None, :], 0.0)
        + jnp.where(second, route_weights[:, 1][None, :], 0.0),
        axis=1,
    ).reshape(groups, slot_span)
    own_rows = lax.dynamic_slice_in_dim(normed, lane * quarter, quarter, axis=1)
    own_cots = lax.dynamic_slice_in_dim(cotangent, lane * quarter, quarter, axis=1)
    sent_rows = jnp.dot(placing, own_rows, preferred_element_type=f32).astype(bf16)
    sent_cots = jnp.dot(placing, own_cots, preferred_element_type=f32).astype(bf16)
    sent_rows = sent_rows.reshape(groups, slot_span, quarter)
    sent_cots = sent_cots.reshape(groups, slot_span, quarter)
    padded = -(-slot_span // 128) * 128
    sent_weights = jnp.broadcast_to(
        jnp.pad(sent_weights, ((0, 0), (0, padded - slot_span)))[:, None, :], (groups, 8, padded)
    )
    got_rows, got_cots, got_weights = dispatch(sent_rows, sent_cots, sent_weights, groups, lanes)
    got_weights = got_weights[:, 0, :slot_span]
    grads_gate, grads_up, grads_down, terms = ([], [], [], [])
    entry_rows = got_rows.reshape(groups * capacity, model_width)
    entry_cots = got_cots.reshape(groups * capacity, model_width)
    entry_weights = got_weights.reshape(groups * capacity)
    grad_gate, grad_up, grad_down, partial_sum = expert_pass(
        entry_rows, entry_cots, entry_weights, gate_weight[0], up_weight[0], down_weight[0]
    )
    grads_gate.append(grad_gate)
    grads_up.append(grad_up)
    grads_down.append(grad_down)
    terms.append(partial_sum.astype(bf16).reshape(groups, capacity, model_width))
    expert_term = terms[0]
    returned = collect(expert_term, groups, lanes).reshape(slots, quarter)
    own_grad = jnp.einsum("st,sq->tq", placing, returned, preferred_element_type=f32)
    dnormed = lax.all_gather(own_grad.astype(bf16), "tp", axis=1, tiled=True).astype(f32)
    scaled = dnormed * norm_gain
    resid_grad = (
        cotangent.astype(f32)
        + inv_rms * scaled
        - resid_wide * inv_rms**3 * jnp.mean(scaled * resid_wide, axis=1, keepdims=True)
    )
    grad_resid = resid_grad.astype(bf16)
    extended = jnp.concatenate([earlier, mixed], axis=0)
    conv = (
        taps[0] * extended[:token_count]
        + taps[1] * extended[1 : token_count + 1]
        + taps[2] * extended[2 : token_count + 2]
    )
    merged = (gate_b.astype(f32) * conv).astype(bf16)
    grad_out_weight = lax.psum_scatter(
        jnp.einsum("td,tc->dc", grad_resid, merged, preferred_element_type=f32).astype(
            jnp.bfloat16
        ),
        "sp",
        scatter_dimension=0,
        tiled=True,
    ).astype(jnp.float32)
    dmerged = jnp.dot(grad_resid, out_weight, preferred_element_type=f32)
    grad_gate_b = (dmerged * conv).astype(bf16)
    dconv = dmerged * gate_b.astype(f32)
    later = passed_along(dconv[:2], "sp", -1)
    extended_grad = jnp.concatenate([dconv, later], axis=0)
    dmixed = (
        taps[2] * extended_grad[:token_count]
        + taps[1] * extended_grad[1 : token_count + 1]
        + taps[0] * extended_grad[2 : token_count + 2]
    )
    grad_gate_c = (dmixed * values_u.astype(f32)).astype(bf16)
    grad_values = (dmixed * gate_c.astype(f32)).astype(bf16)
    return (
        jnp.stack(grads_gate),
        jnp.stack(grads_up),
        jnp.stack(grads_down),
        grad_resid,
        grad_out_weight,
        grad_gate_b,
        grad_gate_c,
        grad_values,
    )


def solution(mesh):
    placed = (
        P("sp", None),
        P("sp", None),
        P(),
        P("sp", None),
        P("sp", None),
        P("sp", None, "tp"),
        P("sp", None, "tp"),
        P("sp", "tp", None),
        P(None, "tp"),
        P("sp", "tp"),
        P("sp", "tp"),
        P("sp", "tp"),
        P(None, "tp"),
    )
    return jax.shard_map(
        on_device,
        mesh=mesh,
        in_specs=placed,
        out_specs=(
            P("sp", None, "tp"),
            P("sp", None, "tp"),
            P("sp", "tp", None),
            P("sp", None),
            P("sp", "tp"),
            P("sp", "tp"),
            P("sp", "tp"),
            P("sp", "tp"),
        ),
        check_vma=False,
    )
```

```python
import functools

import jax
import jax.numpy as jnp
from jax import lax
from jax.experimental import pallas as pl
from jax.experimental.pallas import tpu as pltpu
from jax.sharding import PartitionSpec as P

norm_eps = 1e-06


def passed_along(array, axis, by):
    size = lax.axis_size(axis)
    pairs = [(i, i + by) for i in range(size) if 0 <= i + by < size]
    return lax.ppermute(array, axis, pairs)


def remote(source, target, send_sem, recv_sem, **device):
    return pltpu.make_async_remote_copy(
        src_ref=source,
        dst_ref=target,
        send_sem=send_sem,
        recv_sem=recv_sem,
        device_id=device,
        device_id_type=pl.DeviceIdType.MESH,
    )


def greet(groups, spot, core_peer, far_peer):
    barrier = pltpu.get_barrier_semaphore()

    def to_group(offset, carry):
        pl.semaphore_signal(
            barrier,
            inc=1,
            device_id={"sp": lax.rem(spot + offset, groups)},
            device_id_type=pl.DeviceIdType.MESH,
        )
        return carry

    lax.fori_loop(1, groups, to_group, 0)
    for peer in (core_peer, far_peer):
        pl.semaphore_signal(
            barrier, inc=1, device_id={"tp": peer}, device_id_type=pl.DeviceIdType.MESH
        )
    pl.semaphore_wait(barrier, groups + 1)


def dispatch_kernel(
    groups,
    lanes,
    sent_rows,
    sent_cots,
    sent_weights,
    got_rows,
    got_cots,
    got_weights,
    local_sem,
    send_a,
    recv_a,
    send_x,
    recv_x,
    send_c,
    recv_c,
    send_f,
    recv_f,
    send_w,
    recv_w,
):
    spot, lane = lax.axis_index("sp"), lax.axis_index("tp")
    core_peer = lane + 1 - 2 * lax.rem(lane, 2)
    far_peer = lax.rem(lane + lanes // 2, lanes)
    quarter = sent_rows.shape[2]
    pairs = ((sent_rows, got_rows), (sent_cots, got_cots))

    def part(ref, block, who):
        return ref.at[block, :, pl.ds(pl.multiple_of(who * quarter, quarter), quarter)]

    def across(k, offset):
        goal = lax.rem(spot + offset, groups)
        return remote(
            pairs[k][0].at[goal],
            part(pairs[k][1], spot, lane),
            send_a.at[k, offset],
            recv_a.at[k, offset],
            sp=goal,
        )

    def weights_across(offset):
        goal = lax.rem(spot + offset, groups)
        return remote(
            sent_weights.at[goal],
            got_weights.at[spot],
            send_w.at[offset],
            recv_w.at[offset],
            sp=goal,
        )

    def origin(offset):
        return lax.rem(spot - offset + groups, groups)

    def sideways(k, offset, source, far):
        sems = (send_x, recv_x) if far else (send_c, recv_c)
        return remote(
            source,
            part(pairs[k][1], origin(offset), lane),
            sems[0].at[k, offset],
            sems[1].at[k, offset],
            tp=far_peer if far else core_peer,
        )

    def forward(k, offset):
        held = part(pairs[k][1], origin(offset), far_peer)
        return remote(held, held, send_f.at[k, offset], recv_f.at[k, offset], tp=core_peer)

    greet(groups, spot, core_peer, far_peer)
    own = [
        pltpu.make_async_copy(
            pairs[k][0].at[spot], part(pairs[k][1], spot, lane), local_sem.at[k]
        )
        for k in (0, 1)
    ]
    own_weights = pltpu.make_async_copy(
        sent_weights.at[spot], got_weights.at[spot], local_sem.at[2]
    )

    def launch(offset, carry):
        weights_across(offset).start()
        for k in (0, 1):
            across(k, offset).start()
        return carry

    lax.fori_loop(1, groups, launch, 0)
    for k in (0, 1):
        for far in (True, False):
            sideways(k, 0, pairs[k][0].at[spot], far).start()
    for copy in own:
        copy.start()
    own_weights.start()

    def pass_on(offset, carry):
        for k in (0, 1):
            across(k, offset).wait_recv()
            for far in (True, False):
                sideways(k, offset, part(pairs[k][1], origin(offset), lane), far).start()
        for k in (0, 1):
            sideways(k, offset - 1, part(pairs[k][1], origin(offset - 1), lane), True).wait_recv()
            forward(k, offset - 1).start()
        return carry

    lax.fori_loop(1, groups, pass_on, 0)
    for k in (0, 1):
        last = groups - 1
        sideways(k, last, part(pairs[k][1], origin(last), lane), True).wait_recv()
        forward(k, last).start()

    def finish(offset, carry):
        for k in (0, 1):
            mine = part(pairs[k][1], origin(offset), lane)
            sideways(k, offset, mine, True).wait_send()
            sideways(k, offset, mine, False).wait()
            forward(k, offset).wait()
        return carry

    def finish_across(offset, carry):
        weights_across(offset).wait()
        for k in (0, 1):
            across(k, offset).wait_send()
        return carry

    lax.fori_loop(0, groups, finish, 0)
    lax.fori_loop(1, groups, finish_across, 0)
    for copy in own:
        copy.wait()
    own_weights.wait()


def dispatch(sent_rows, sent_cots, sent_weights, groups, lanes):
    span, quarter = sent_rows.shape[1:]
    whole = jax.ShapeDtypeStruct((groups, span, quarter * lanes), sent_rows.dtype)
    sem = pltpu.SemaphoreType.DMA
    anywhere = pl.BlockSpec(memory_space=pl.ANY)
    wire = 2 * span * quarter * 2 * groups * 3
    return pl.pallas_call(
        functools.partial(dispatch_kernel, groups, lanes),
        out_shape=(
            whole,
            whole,
            jax.ShapeDtypeStruct(sent_weights.shape, sent_weights.dtype),
        ),
        in_specs=[anywhere] * 3,
        out_specs=(anywhere,) * 3,
        scratch_shapes=[sem((3,))] + [sem((2, groups))] * 8 + [sem((groups,))] * 2,
        compiler_params=pltpu.CompilerParams(collective_id=1, has_side_effects=True),
        cost_estimate=pl.CostEstimate(
            flops=0, bytes_accessed=40 * wire, transcendentals=0
        ),
        name="dispatch",
    )(sent_rows, sent_cots, sent_weights)


def collect_kernel(
    groups,
    lanes,
    partial,
    returned,
    from_core,
    to_far,
    from_far,
    summed,
    send_c,
    recv_c,
    send_x,
    recv_x,
    send_a,
    recv_a,
):
    f32 = jnp.float32
    bf16 = jnp.bfloat16
    spot, lane = lax.axis_index("sp"), lax.axis_index("tp")
    core_peer = lane + 1 - 2 * lax.rem(lane, 2)
    far_peer = lax.rem(lane + lanes // 2, lanes)
    quarter = returned.shape[2]

    def part(block, who):
        return partial.at[block, :, pl.ds(pl.multiple_of(who * quarter, quarter), quarter)]

    def goal_of(step):
        return lax.rem(spot + step + 1, groups)

    def to_core(step, far):
        who = lax.rem(core_peer + far * (lanes // 2), lanes)
        return remote(
            part(goal_of(step), who),
            from_core.at[step, far],
            send_c.at[step, far],
            recv_c.at[step, far],
            tp=core_peer,
        )

    def to_far_peer(step):
        return remote(
            to_far.at[step], from_far.at[step], send_x.at[step], recv_x.at[step], tp=far_peer
        )

    def home(step):
        goal = goal_of(step)
        return remote(
            summed.at[step], returned.at[spot], send_a.at[step], recv_a.at[step], sp=goal
        )

    greet(groups, spot, core_peer, far_peer)

    def begin(step, carry):
        to_core(step, 1).start()
        to_core(step, 0).start()
        return carry

    lax.fori_loop(0, groups, begin, 0)

    def middle(step, carry):
        to_core(step, 1).wait_recv()
        to_far[step] = (
            part(goal_of(step), far_peer)[...].astype(f32) + from_core[step, 1].astype(f32)
        ).astype(bf16)
        to_far_peer(step).start()
        return carry

    lax.fori_loop(0, groups, middle, 0)

    def total(step):
        to_core(step, 0).wait_recv()
        to_far_peer(step).wait_recv()
        return (
            part(goal_of(step), lane)[...].astype(f32)
            + from_core[step, 0].astype(f32)
            + from_far[step].astype(f32)
        ).astype(bf16)

    def end(step, carry):
        summed[step] = total(step)
        home(step).start()
        return carry

    lax.fori_loop(0, groups - 1, end, 0)
    returned[spot] = total(groups - 1)

    def finish(step, carry):
        to_core(step, 0).wait_send()
        to_core(step, 1).wait_send()
        to_far_peer(step).wait_send()
        return carry

    lax.fori_loop(0, groups, finish, 0)

    def finish_home(step, carry):
        home(step).wait()
        return carry

    lax.fori_loop(0, groups - 1, finish_home, 0)


def collect(partial, groups, lanes):
    span, width = partial.shape[1:]
    quarter = width // lanes
    block = (groups, span, quarter)
    sem = pltpu.SemaphoreType.DMA
    inside = pl.BlockSpec(memory_space=pltpu.VMEM)
    return pl.pallas_call(
        functools.partial(collect_kernel, groups, lanes),
        out_shape=jax.ShapeDtypeStruct(block, partial.dtype),
        in_specs=[inside],
        out_specs=inside,
        scratch_shapes=[
            pltpu.VMEM((groups, 2, span, quarter), partial.dtype),
            pltpu.VMEM(block, partial.dtype),
            pltpu.VMEM(block, partial.dtype),
            pltpu.VMEM(block, partial.dtype),
            sem((groups, 2)),
            sem((groups, 2)),
        ]
        + [sem((groups,))] * 4,
        compiler_params=pltpu.CompilerParams(
            collective_id=2, has_side_effects=True, vmem_limit_bytes=40 * 2**20
        ),
        cost_estimate=pl.CostEstimate(
            flops=0, bytes_accessed=150 * 2**20, transcendentals=0
        ),
        name="collect",
    )(partial)


def gather_kernel(groups, lanes, mine, gathered, own_sem, send_sems, recv_sems):
    spot, lane = lax.axis_index("sp"), lax.axis_index("tp")
    core_peer = lane + 1 - 2 * lax.rem(lane, 2)
    far_peer = lax.rem(lane + lanes // 2, lanes)
    quarter = mine.shape[1]

    def part(who):
        return gathered.at[:, pl.ds(pl.multiple_of(who * quarter, quarter), quarter)]

    greet(groups, spot, core_peer, far_peer)
    far = remote(mine, part(lane), send_sems.at[0], recv_sems.at[0], tp=far_peer)
    near = remote(mine, part(lane), send_sems.at[1], recv_sems.at[1], tp=core_peer)
    own = pltpu.make_async_copy(mine, part(lane), own_sem)
    far.start()
    near.start()
    own.start()
    far.wait_recv()
    passed = remote(
        part(far_peer), part(far_peer), send_sems.at[2], recv_sems.at[2], tp=core_peer
    )
    passed.start()
    far.wait_send()
    near.wait()
    own.wait()
    passed.wait()


def gather_quarters(mine, groups, lanes):
    sem = pltpu.SemaphoreType.DMA
    inside = pl.BlockSpec(memory_space=pltpu.VMEM)
    return pl.pallas_call(
        functools.partial(gather_kernel, groups, lanes),
        out_shape=jax.ShapeDtypeStruct((mine.shape[0], mine.shape[1] * lanes), mine.dtype),
        in_specs=[inside],
        out_specs=inside,
        scratch_shapes=[sem, sem((3,)), sem((3,))],
        compiler_params=pltpu.CompilerParams(collective_id=3, has_side_effects=True),
        name="gather_quarters",
    )(mine)


def reduce_kernel(groups, lanes, partial, total, arrived, send_sems, recv_sems):
    f32 = jnp.float32
    spot, lane = lax.axis_index("sp"), lax.axis_index("tp")
    core_peer = lane + 1 - 2 * lax.rem(lane, 2)
    far_peer = lax.rem(lane + lanes // 2, lanes)

    def across(offset):
        goal = lax.rem(spot + offset, groups)
        return remote(
            partial.at[goal],
            arrived.at[offset],
            send_sems.at[offset],
            recv_sems.at[offset],
            sp=goal,
        )

    greet(groups, spot, core_peer, far_peer)

    def launch(offset, carry):
        across(offset).start()
        return carry

    lax.fori_loop(1, groups, launch, 0)
    total[...] = partial[spot].astype(f32)

    def add(offset, carry):
        across(offset).wait_recv()
        total[...] += arrived[offset].astype(f32)
        return carry

    lax.fori_loop(1, groups, add, 0)

    def finish(offset, carry):
        across(offset).wait_send()
        return carry

    lax.fori_loop(1, groups, finish, 0)


def reduce_rows(partial, groups, lanes):
    sem = pltpu.SemaphoreType.DMA
    inside = pl.BlockSpec(memory_space=pltpu.VMEM)
    return pl.pallas_call(
        functools.partial(reduce_kernel, groups, lanes),
        out_shape=jax.ShapeDtypeStruct(partial.shape[1:], jnp.float32),
        in_specs=[inside],
        out_specs=inside,
        scratch_shapes=[
            pltpu.VMEM(partial.shape, partial.dtype),
            sem((groups,)),
            sem((groups,)),
        ],
        compiler_params=pltpu.CompilerParams(collective_id=4, has_side_effects=True),
        name="reduce_rows",
    )(partial)


def expert_pass(entry_rows, entry_cots, entry_weights, gate_mat, up_mat, down_mat):
    f32 = jnp.float32
    bf16 = jnp.bfloat16
    gate_pre = jnp.dot(entry_rows, gate_mat, preferred_element_type=f32)
    up_pre = jnp.dot(entry_rows, up_mat, preferred_element_type=f32)
    logistic = jax.nn.sigmoid(gate_pre)
    activated = gate_pre * logistic
    hidden = (activated * up_pre * entry_weights[:, None]).astype(bf16)
    grad_down = jnp.einsum("rf,rd->fd", hidden, entry_cots, preferred_element_type=f32)
    dhidden = (
        jnp.einsum("rd,fd->rf", entry_cots, down_mat, preferred_element_type=f32)
        * entry_weights[:, None]
    )
    dgate = (dhidden * up_pre * logistic * (1.0 + gate_pre * (1.0 - logistic))).astype(bf16)
    dup = (dhidden * activated).astype(bf16)
    grad_gate = jnp.einsum("rd,rf->df", entry_rows, dgate, preferred_element_type=f32)
    grad_up = jnp.einsum("rd,rf->df", entry_rows, dup, preferred_element_type=f32)
    partial_sum = jnp.einsum("rf,df->rd", dgate, gate_mat, preferred_element_type=f32) + jnp.einsum(
        "rf,df->rd", dup, up_mat, preferred_element_type=f32
    )
    return (grad_gate, grad_up, grad_down, partial_sum)


def on_device(
    resid_in,
    cotangent,
    norm_gain,
    routes,
    route_weights,
    gate_weight,
    up_weight,
    down_weight,
    out_weight,
    gate_b,
    gate_c,
    values_u,
    taps,
):
    f32 = jnp.float32
    bf16 = jnp.bfloat16
    token_count, model_width = resid_in.shape
    groups = lax.axis_size("sp")
    lanes = lax.axis_size("tp")
    local_experts = gate_weight.shape[0]
    expert_total = local_experts * groups
    capacity = 4 * token_count // expert_total
    slot_span = local_experts * capacity
    resid_wide = resid_in.astype(f32)
    inv_rms = lax.rsqrt(jnp.mean(resid_wide * resid_wide, axis=1, keepdims=True) + norm_eps)
    normed = (resid_wide * inv_rms * norm_gain).astype(bf16)
    mixed = gate_c.astype(f32) * values_u.astype(f32)
    earlier = passed_along(mixed[-2:], "sp", 1)
    quarter = model_width // lanes
    lane = lax.axis_index("tp")
    slots = expert_total * capacity
    names = jnp.arange(expert_total, dtype=jnp.int32)
    chosen = routes[:, :, None] == names[None, None, :]
    named = jnp.any(chosen, axis=1).astype(bf16)
    order = jnp.arange(token_count, dtype=jnp.int32)
    strict = (order[:, None] > order[None, :]).astype(bf16)
    before = jnp.dot(strict, named, preferred_element_type=f32).astype(jnp.int32)
    rank = jnp.sum(jnp.where(chosen, before[:, None, :], 0), axis=2)
    targets = routes * capacity + rank
    slot_ids = jnp.arange(slots, dtype=jnp.int32)[:, None]
    first = slot_ids == targets[:, 0][None, :]
    second = slot_ids == targets[:, 1][None, :]
    placing = (first | second).astype(bf16)
    sent_weights = jnp.sum(
        jnp.where(first, route_weights[:, 0][None, :], 0.0)
        + jnp.where(second, route_weights[:, 1][None, :], 0.0),
        axis=1,
    ).reshape(groups, slot_span)
    own_rows = lax.dynamic_slice_in_dim(normed, lane * quarter, quarter, axis=1)
    own_cots = lax.dynamic_slice_in_dim(cotangent, lane * quarter, quarter, axis=1)
    sent_rows = jnp.dot(placing, own_rows, preferred_element_type=f32).astype(bf16)
    sent_cots = jnp.dot(placing, own_cots, preferred_element_type=f32).astype(bf16)
    sent_rows = sent_rows.reshape(groups, slot_span, quarter)
    sent_cots = sent_cots.reshape(groups, slot_span, quarter)
    padded = -(-slot_span // 128) * 128
    sent_weights = jnp.broadcast_to(
        jnp.pad(sent_weights, ((0, 0), (0, padded - slot_span)))[:, None, :], (groups, 8, padded)
    )
    got_rows, got_cots, got_weights = dispatch(sent_rows, sent_cots, sent_weights, groups, lanes)
    got_weights = got_weights[:, 0, :slot_span]
    grads_gate, grads_up, grads_down, terms = ([], [], [], [])
    entry_rows = got_rows.reshape(groups * capacity, model_width)
    entry_cots = got_cots.reshape(groups * capacity, model_width)
    entry_weights = got_weights.reshape(groups * capacity)
    grad_gate, grad_up, grad_down, partial_sum = expert_pass(
        entry_rows, entry_cots, entry_weights, gate_weight[0], up_weight[0], down_weight[0]
    )
    grads_gate.append(grad_gate)
    grads_up.append(grad_up)
    grads_down.append(grad_down)
    terms.append(partial_sum.astype(bf16).reshape(groups, capacity, model_width))
    expert_term = terms[0]
    returned = collect(expert_term, groups, lanes).reshape(slots, quarter)
    own_grad = jnp.einsum("st,sq->tq", placing, returned, preferred_element_type=f32)
    dnormed = gather_quarters(own_grad.astype(bf16), groups, lanes).astype(f32)
    scaled = dnormed * norm_gain
    resid_grad = (
        cotangent.astype(f32)
        + inv_rms * scaled
        - resid_wide * inv_rms**3 * jnp.mean(scaled * resid_wide, axis=1, keepdims=True)
    )
    grad_resid = resid_grad.astype(bf16)
    extended = jnp.concatenate([earlier, mixed], axis=0)
    conv = (
        taps[0] * extended[:token_count]
        + taps[1] * extended[1 : token_count + 1]
        + taps[2] * extended[2 : token_count + 2]
    )
    merged = (gate_b.astype(f32) * conv).astype(bf16)
    out_partial = jnp.einsum("td,tc->dc", grad_resid, merged, preferred_element_type=f32)
    grad_out_weight = reduce_rows(
        out_partial.astype(bf16).reshape(groups, model_width // groups, merged.shape[1]),
        groups,
        lanes,
    )
    dmerged = jnp.dot(grad_resid, out_weight, preferred_element_type=f32)
    grad_gate_b = (dmerged * conv).astype(bf16)
    dconv = dmerged * gate_b.astype(f32)
    later = passed_along(dconv[:2], "sp", -1)
    extended_grad = jnp.concatenate([dconv, later], axis=0)
    dmixed = (
        taps[2] * extended_grad[:token_count]
        + taps[1] * extended_grad[1 : token_count + 1]
        + taps[0] * extended_grad[2 : token_count + 2]
    )
    grad_gate_c = (dmixed * values_u.astype(f32)).astype(bf16)
    grad_values = (dmixed * gate_c.astype(f32)).astype(bf16)
    return (
        jnp.stack(grads_gate),
        jnp.stack(grads_up),
        jnp.stack(grads_down),
        grad_resid,
        grad_out_weight,
        grad_gate_b,
        grad_gate_c,
        grad_values,
    )


def solution(mesh):
    placed = (
        P("sp", None),
        P("sp", None),
        P(),
        P("sp", None),
        P("sp", None),
        P("sp", None, "tp"),
        P("sp", None, "tp"),
        P("sp", "tp", None),
        P(None, "tp"),
        P("sp", "tp"),
        P("sp", "tp"),
        P("sp", "tp"),
        P(None, "tp"),
    )
    return jax.shard_map(
        on_device,
        mesh=mesh,
        in_specs=placed,
        out_specs=(
            P("sp", None, "tp"),
            P("sp", None, "tp"),
            P("sp", "tp", None),
            P("sp", None),
            P("sp", "tp"),
            P("sp", "tp"),
            P("sp", "tp"),
            P("sp", "tp"),
        ),
        check_vma=False,
    )
```
